32 devices in a mesh: fs: 16 (over z, y, x), tp: 2 (over core).
Axes of the slice: x: 2, y: 2, z: 4, core: 2. Of those that a mesh axis runs over, the one named last changes fastest.
Arguments:
- tokens: bfloat16 [3072, 2048], P('fs'), may hold values from -6 to 6
- route_ids: int32 [3072, 2], P('fs'), may hold values from 0 to 7, all different within a row; in each aligned block of 192 rows (0 to 191, 192 to 383, ...) at most 96 rows name the same one
- route_logits: float32 [3072, 2], P('fs'), may hold values from -6 to 6
- norm_gain: float32 [2048], P('fs'), may hold values from 0.1 to 1.9
- gate_weight: float32 [8, 2048, 2048], P(None, 'fs', 'tp'), may hold values from -0.125 to 0.125
- up_weight: float32 [8, 2048, 2048], P(None, 'fs', 'tp'), may hold values from -0.125 to 0.125
- down_weight: float32 [8, 2048, 2048], P(None, 'fs', 'tp'), may hold values from -0.125 to 0.125
Outputs:
- mixed: bfloat16 [3072, 2048], P('fs')
- gate_copies: bfloat16 [16, 2048, 2048], P('fs', None, 'tp')
- up_copies: bfloat16 [16, 2048, 2048], P('fs', None, 'tp')
- down_copies: bfloat16 [16, 2048, 2048], P('fs', None, 'tp')
The draws below stay inside these ranges and needn't reach their ends.
Inputs may be any that keep to these rules, and one draw needn't show every extreme that they name: `route_ids`: each row names 2 different experts. Among the rows of one index of fs no expert is named by more than 96 rows, a bound that some of them reach.
All inputs are finite; a program needn't handle non-finite values.
Results may differ from the reference program's by a relative error of at most 0.014.
Values may be sent and summed in bfloat16 or wider, within the bound.
No kernel may reach another device: no remote copies, remote signals or barrier semaphores. Data moves between devices by JAX's collectives and lax.ppermute only.
A program may use at most 128 MiB of HBM per device.

```python
import math
import jax
import jax.numpy as jnp
import numpy as np
from jax import lax

D = 2048
FF = 2048
EXPERTS = 8
TOP = 2
TOK_DEV = 192
CAP = 96
TOKENS = 3072
N_FS = 16
N_TP = 2


def levels(key, extent, split, low, high):
    def one(dim, blocks):
        steps = jax.random.uniform(jax.random.fold_in(jax.random.fold_in(key, 6), dim), (blocks,), jnp.float32, low / len(split), high / len(split))
        return jnp.repeat(jnp.exp(steps), extent[dim] // blocks).reshape((-1,) + (1,) * (len(extent) - dim - 1))

    level = one(*split[0])
    for cut in split[1:]:
        level = level * one(*cut)
    return level


def deal_out(rng, own, number, rows, number_of, top, most, lean):
    ranking = jax.random.permutation(rng, number_of)
    packed, usual = load_shares(number_of, rows * top, most, lean, True), load_shares(number_of, rows * top, most, lean, False)
    places = jnp.arange(number_of)

    def named(tallies, rotation):
        used = int((tallies > 0).sum())
        fixed = max(1, used // 4)
        moved = fixed + (places - fixed + rotation * (used - fixed)) % max(1, number_of - fixed)
        return jnp.zeros((number_of,), jnp.int32).at[ranking[jnp.where(places < fixed, places, moved)]].set(jnp.asarray(tallies, jnp.int32))

    tallies = jnp.where(number % 4 == 0, named(packed, number // 4), named(usual, number - number // 4 - 1))
    mixed = jax.random.permutation(jax.random.fold_in(own, 3), number_of)
    donor, sink = mixed[0:number_of // 2 * 2:2], mixed[1:number_of // 2 * 2:2]
    margin = jnp.minimum(tallies[donor] - 1, most - tallies[sink]) // 2
    margin = jnp.where((donor == ranking[0]) | (sink == ranking[0]) | (tallies[sink] == 0), 0, jnp.maximum(margin, 0))
    moved = jax.random.randint(jax.random.fold_in(own, 4), (number_of // 2,), 0, 1 << 20) % (margin + 1)
    tallies = tallies.at[donor].add(-moved).at[sink].add(moved)
    labels = jnp.searchsorted(jnp.cumsum(tallies), jnp.arange(rows * top), side="right").astype(jnp.int32)
    grid = labels.reshape(top, rows).T
    grid = grid[jax.random.permutation(jax.random.fold_in(own, 1), rows)]
    rotation = jax.random.randint(jax.random.fold_in(own, 2), (rows, 1), 0, top)
    return jnp.take_along_axis(grid, (jnp.arange(top)[None, :] + rotation) % top, axis=1)


def load_shares(amount, total, reach, skew, full):
    weights = [(1 << 20) // math.isqrt(rank ** skew) + 1 for rank in range(1, amount + 1)]
    largest = reach if full else min(reach, max(-(-total // amount), total * weights[0] // sum(weights)))
    least = 1 if total - largest >= amount - 1 else 0
    given, rest = [largest] + [least] * (amount - 1), total - largest - least * (amount - 1)
    while rest > 0:
        candidates = [i for i in range(1, amount) if given[i] < largest] or [i for i in range(1, amount) if given[i] < reach]
        pool, left = sum([weights[i] for i in candidates]), rest
        for i in candidates:
            more = min(reach - given[i], max(1, left * weights[i] // pool), rest)
            given[i] = given[i] + more
            rest = rest - more
    return np.array(given)


def centred(stream_key, extent, deviation, limit, cuts=(), held_as=jnp.bfloat16):
    result = deviation * jax.random.normal(stream_key, extent, jnp.float32)
    if cuts:
        result = result * levels(stream_key, extent, cuts, -0.22, 0.18)
    return jnp.clip(result, -limit, limit).astype(held_as)


def setup_inputs(seed: int = 0) -> dict:
    seeds = jax.random.split(jax.random.key(seed), 8)
    tokens = centred(seeds[0], (TOKENS, D), 1.0, 6.0, ((0, 16),))
    route_ids_keys = jax.random.split(jax.random.fold_in(seeds[1], 1), TOKENS // TOK_DEV)
    route_ids_turns = jax.random.permutation(jax.random.fold_in(seeds[1], 3), TOKENS // TOK_DEV)
    route_ids = jax.vmap(lambda own, number: deal_out(jax.random.fold_in(seeds[1], 2), own, number, TOK_DEV, EXPERTS, TOP, CAP, 1))(route_ids_keys, route_ids_turns).reshape((TOKENS, TOP))
    route_logits = centred(seeds[2], (TOKENS, TOP), 1.5, 6.0, ((0, 16),), jnp.float32)
    norm_gain = jnp.clip(1.0 + 0.18 * jax.random.normal(seeds[3], (D,), jnp.float32), 0.1, 1.9)
    gate_weight = centred(seeds[4], (EXPERTS, D, FF), D ** -0.5, 0.125, ((1, 16), (2, 2)), jnp.float32)
    up_weight = centred(seeds[5], (EXPERTS, D, FF), D ** -0.5, 0.125, ((1, 16), (2, 2)), jnp.float32)
    down_weight = centred(seeds[6], (EXPERTS, D, FF), FF ** -0.5, 0.125, ((1, 16), (2, 2)), jnp.float32)
    return dict(tokens=tokens, route_ids=route_ids, route_logits=route_logits, norm_gain=norm_gain, gate_weight=gate_weight, up_weight=up_weight, down_weight=down_weight)


def expert_rows(rows, gate_matrix, up_matrix, down_matrix):
    gate_act = jnp.dot(rows, gate_matrix, preferred_element_type=jnp.float32)
    up_act = jnp.dot(rows, up_matrix, preferred_element_type=jnp.float32)
    hidden = (jax.nn.silu(gate_act) * up_act).astype(jnp.bfloat16)
    row_count = rows.shape[0]
    blocks = hidden.reshape(row_count, N_TP, FF // N_TP).astype(jnp.float32)
    down_blocks = down_matrix.reshape(D, N_TP, FF // N_TP).astype(jnp.float32)
    partial_value = jnp.einsum('rbf,dbf->brd', blocks, down_blocks)
    rounded = lax.optimization_barrier(partial_value.astype(jnp.bfloat16))
    return lax.optimization_barrier(jnp.sum(rounded.astype(jnp.float32), axis=0)).astype(jnp.bfloat16)

def reference(tokens, route_ids, route_logits, norm_gain, gate_weight, up_weight, down_weight):
    copies = N_FS // EXPERTS
    folded_gate = (norm_gain[None, :, None] * gate_weight).astype(jnp.bfloat16)
    folded_up = (norm_gain[None, :, None] * up_weight).astype(jnp.bfloat16)
    down_cast = down_weight.astype(jnp.bfloat16)
    gate_copies = jnp.repeat(folded_gate, copies, axis=0)
    up_copies = jnp.repeat(folded_up, copies, axis=0)
    down_copies = jnp.repeat(down_cast, copies, axis=0)
    values = tokens.astype(jnp.float32)
    center = lax.optimization_barrier(jnp.mean(values, axis=1, keepdims=True))
    spread = lax.optimization_barrier(jnp.mean(jnp.square(values - center), axis=1, keepdims=True))
    normed = ((values - center) * lax.rsqrt(spread + 1e-06)).astype(jnp.bfloat16)
    per_source = route_ids.reshape(N_FS, TOK_DEV * TOP)
    onehot_table = (per_source[:, :, None] == jnp.arange(EXPERTS, dtype=jnp.int32)[None, None, :]).astype(jnp.int32)
    before = jnp.cumsum(onehot_table, axis=1) - onehot_table
    order_rank = lax.optimization_barrier(jnp.sum(before * onehot_table, axis=2))
    source = jnp.arange(N_FS, dtype=jnp.int32)[:, None]
    position = source * CAP + order_rank
    owners = source * TOK_DEV + jnp.arange(TOK_DEV * TOP, dtype=jnp.int32)[None, :] // TOP
    slot_token = jnp.full((EXPERTS, N_FS * CAP), TOKENS, jnp.int32).at[per_source, position].set(owners)
    padded = jnp.concatenate([normed, jnp.zeros((1, D), jnp.bfloat16)], axis=0)

    def one_expert(index):
        rows = padded[slot_token[index]]
        return expert_rows(rows, folded_gate[index], folded_up[index], down_cast[index])
    results = lax.map(one_expert, jnp.arange(EXPERTS, dtype=jnp.int32))
    picked = results[per_source, position].reshape(TOKENS, TOP, D).astype(jnp.float32)
    first_weight = jax.nn.sigmoid(route_logits[:, 0] - route_logits[:, 1])
    second_weight = jax.nn.sigmoid(route_logits[:, 1] - route_logits[:, 0])
    mixed = (first_weight[:, None] * picked[:, 0] + second_weight[:, None] * picked[:, 1]).astype(jnp.bfloat16)
    return (mixed, gate_copies, up_copies, down_copies)
```

```python
import jax
import jax.numpy as jnp
from jax import lax
from jax.sharding import PartitionSpec as P

CAP = 96


def after(value, *earlier):
    return lax.optimization_barrier((value,) + earlier)[0]


def body(tokens, route_ids, route_logits, norm_gain, gate_weight, up_weight, down_weight):
    experts = gate_weight.shape[0]
    fs_count = lax.axis_size("fs")
    tp_count = lax.axis_size("tp")
    copies = fs_count // experts
    width = tokens.shape[1]
    lane = lax.axis_index("fs") % copies
    tp_index = lax.axis_index("tp")
    planes = [[e * copies + c for e in range(experts)] for c in range(copies)]

    def exchange(value):
        return lax.all_to_all(
            value, "fs", split_axis=0, concat_axis=0, tiled=True, axis_index_groups=planes
        )

    def hand_round(value):
        return [
            lax.ppermute(
                value,
                "fs",
                [
                    (e * copies + c, e * copies + (c + step) % copies)
                    for e in range(experts)
                    for c in range(copies)
                ],
            )
            for step in range(1, copies)
        ]

    def weave(own, others):
        if copies == 2:
            parts = [
                jnp.where(lane == 0, own, others[0]),
                jnp.where(lane == 0, others[0], own),
            ]
            joined = jnp.stack(parts, axis=1)
        else:
            held = jnp.stack([own] + others)
            joined = jnp.moveaxis(held[(lane - jnp.arange(copies)) % copies], 0, 1)
        return joined.reshape(1, -1, own.shape[-1])

    def other_core(value):
        return lax.ppermute(value, "tp", [(0, 1), (1, 0)])

    def join_cols(part):
        if tp_count == 2:
            other = other_core(part)
            return jnp.where(
                tp_index == 0,
                jnp.concatenate([part, other], axis=1),
                jnp.concatenate([other, part], axis=1),
            )
        return lax.all_gather(part, "tp", axis=1, tiled=True)

    def sum_cols(partial):
        if tp_count == 2:
            half = partial.shape[1] // 2
            low, high = partial[:, :half], partial[:, half:]
            kept = jnp.where(tp_index == 0, low, high)
            given = jnp.where(tp_index == 0, high, low)
            return (kept.astype(jnp.float32) + other_core(given).astype(jnp.float32)).astype(
                jnp.bfloat16
            )
        return lax.psum_scatter(partial, "tp", scatter_dimension=1, tiled=True)

    scaled_gain = norm_gain[None, :, None]
    gate_own = exchange((scaled_gain * gate_weight).astype(jnp.bfloat16))
    gate_others = hand_round(gate_own)

    values = tokens.astype(jnp.float32)
    center = jnp.mean(values, axis=1, keepdims=True)
    spread = jnp.mean(jnp.square(values - center), axis=1, keepdims=True)
    normed = ((values - center) * lax.rsqrt(spread + 1e-06)).astype(jnp.bfloat16)
    rows = tokens.shape[0]
    names = jnp.arange(experts, dtype=jnp.int32)
    named = jnp.any(route_ids[:, :, None] == names[None, None, :], axis=1)
    row_no = jnp.arange(rows, dtype=jnp.int32)
    earlier = (row_no[:, None] > row_no[None, :]).astype(jnp.bfloat16)
    before = jnp.dot(earlier, named.astype(jnp.bfloat16), preferred_element_type=jnp.float32)
    place = jnp.where(named, before.astype(jnp.int32), CAP)
    slots = jnp.arange(CAP, dtype=jnp.int32)
    pick = (place.T[:, None, :] == slots[None, :, None]).astype(jnp.bfloat16)
    pick = pick.reshape(experts * CAP, rows)
    col_count = width // tp_count
    own_cols = lax.dynamic_slice_in_dim(normed, tp_index * col_count, col_count, 1)
    send_rows = jnp.dot(pick, own_cols, preferred_element_type=jnp.float32).astype(jnp.bfloat16)

    up_send = (scaled_gain * up_weight).astype(jnp.bfloat16)
    up_own = exchange(after(up_send, gate_own))
    up_others = hand_round(up_own)
    arrived = exchange(after(send_rows.reshape(experts, CAP, col_count), up_own, gate_others[0]))
    piece = join_cols(arrived.reshape(-1, col_count))
    down_send = down_weight.astype(jnp.bfloat16)
    down_own = exchange(after(down_send, arrived, up_others[0]))
    down_others = hand_round(down_own)

    gate_new = weave(gate_own, gate_others)
    up_new = weave(up_own, up_others)
    down_new = weave(down_own, down_others)

    gate_act = jnp.dot(piece, gate_new[0], preferred_element_type=jnp.float32)
    up_act = jnp.dot(piece, up_new[0], preferred_element_type=jnp.float32)
    hidden = (jax.nn.silu(gate_act) * up_act).astype(jnp.bfloat16)
    partial_value = jnp.einsum(
        "rf,df->rd", hidden, down_new[0], preferred_element_type=jnp.float32
    ).astype(jnp.bfloat16)
    share = sum_cols(partial_value)
    returned = exchange(share.reshape(experts, CAP, col_count)).reshape(experts * CAP, col_count)

    def chosen(k):
        spot = jnp.sum(
            jnp.where(route_ids[:, k, None] == names[None, :], place + CAP * names[None, :], 0),
            axis=1,
        )
        hot = (spot[:, None] == jnp.arange(experts * CAP, dtype=jnp.int32)[None, :]).astype(
            jnp.bfloat16
        )
        return jnp.dot(hot, returned, preferred_element_type=jnp.float32)

    first_weight = jax.nn.sigmoid(route_logits[:, 0] - route_logits[:, 1])
    second_weight = jax.nn.sigmoid(route_logits[:, 1] - route_logits[:, 0])
    mixed_cols = (
        first_weight[:, None] * chosen(0) + second_weight[:, None] * chosen(1)
    ).astype(jnp.bfloat16)
    mixed = join_cols(mixed_cols)
    return (mixed, gate_new, up_new, down_new)


def solution(mesh):
    return jax.shard_map(
        body,
        mesh=mesh,
        in_specs=(
            P("fs", None),
            P("fs", None),
            P("fs", None),
            P("fs"),
            P(None, "fs", "tp"),
            P(None, "fs", "tp"),
            P(None, "fs", "tp"),
        ),
        out_specs=(P("fs", None), P("fs", None, "tp"), P("fs", None, "tp"), P("fs", None, "tp")),
        check_vma=False,
    )
```

```python
import functools

import jax
import jax.numpy as jnp
import numpy as np
from jax import lax
from jax.experimental import pallas as pl
from jax.experimental.pallas import tpu as pltpu
from jax.sharding import PartitionSpec as P

CAP = 96


def after(value, *earlier):
    return lax.optimization_barrier((value,) + earlier)[0]


def place_kernel(moves, number, where_ref, *refs):
    arrays, outs = refs[:number], refs[number : -2 - number]
    held = refs[-2 - number : -2]
    in_sems, out_sems = refs[-2:]
    loads = [
        pltpu.make_async_copy(array, held[i], in_sems.at[i]) for i, array in enumerate(arrays)
    ]
    for load in loads:
        load.start()
    stores = []
    seen = set()
    for n, (i, part, first, rows, out, start, slot) in enumerate(moves):
        if i not in seen:
            loads[i].wait()
            seen.add(i)
        store = pltpu.make_async_copy(
            held[i].at[part, pl.ds(first, rows)],
            outs[out].at[where_ref[slot], pl.ds(start, rows)],
            out_sems.at[n],
        )
        store.start()
        stores.append(store)
    for store in stores:
        store.wait()


def place(arrays, moves, where, out_shapes):
    dtype = arrays[0].dtype
    hbm = pl.BlockSpec(memory_space=pltpu.HBM)
    size = 2 * sum(int(np.prod(a.shape)) for a in arrays)
    return pl.pallas_call(
        functools.partial(place_kernel, moves, len(arrays)),
        grid_spec=pltpu.PrefetchScalarGridSpec(
            num_scalar_prefetch=1,
            grid=(),
            in_specs=[hbm] * len(arrays),
            out_specs=[hbm] * len(out_shapes),
            scratch_shapes=[pltpu.VMEM(a.shape, dtype) for a in arrays]
            + [
                pltpu.SemaphoreType.DMA((len(arrays),)),
                pltpu.SemaphoreType.DMA((len(moves),)),
            ],
        ),
        out_shape=[jax.ShapeDtypeStruct(s, dtype) for s in out_shapes],
        cost_estimate=pl.CostEstimate(flops=4 * size, bytes_accessed=2 * size, transcendentals=0),
    )(where, *arrays)


def pick_kernel(layout, cols, where_ref, *refs):
    arrays, out_ref = refs[:-1], refs[-1]
    expert = where_ref[len(layout)]
    slots = lax.broadcasted_iota(jnp.int32, (1, CAP), 1).astype(jnp.float32)
    for n, (i, part) in enumerate(layout):
        block = arrays[i][part]
        extra = block[:, cols:].astype(jnp.float32)
        column = lax.broadcasted_iota(jnp.int32, extra.shape, 1)
        rank = jnp.sum(jnp.where(column == expert, extra, 0.0), axis=1, keepdims=True)
        hot = (rank == slots).astype(jnp.float32).astype(block.dtype)
        rows = lax.dot_general(
            hot, block[:, :cols], (((0,), (0,)), ((), ())), preferred_element_type=jnp.float32
        )
        out_ref[where_ref[n]] = rows.astype(out_ref.dtype)


def pick_rows(arrays, layout, where, cols):
    size = 2 * sum(int(np.prod(a.shape)) for a in arrays)
    rows = arrays[0].shape[1]
    vmem = pl.BlockSpec(memory_space=pltpu.VMEM)
    return pl.pallas_call(
        functools.partial(pick_kernel, layout, cols),
        grid_spec=pltpu.PrefetchScalarGridSpec(
            num_scalar_prefetch=1, grid=(), in_specs=[vmem] * len(arrays), out_specs=vmem
        ),
        out_shape=jax.ShapeDtypeStruct((len(layout), CAP, cols), arrays[0].dtype),
        cost_estimate=pl.CostEstimate(
            flops=2 * len(layout) * CAP * rows * cols, bytes_accessed=2 * size, transcendentals=0
        ),
    )(where, *arrays)


def body(tokens, route_ids, route_logits, norm_gain, gate_weight, up_weight, down_weight):
    experts, depth, cols = gate_weight.shape
    fs_count = lax.axis_size("fs")
    tp_count = lax.axis_size("tp")
    copies = fs_count // experts
    rows, width = tokens.shape
    share_width = width // tp_count
    lane = lax.axis_index("fs") % copies
    expert = lax.axis_index("fs") // copies
    tp_index = lax.axis_index("tp")
    planes = [[e * copies + c for e in range(experts)] for c in range(copies)]

    def exchange(value):
        return lax.all_to_all(
            value, "fs", split_axis=0, concat_axis=0, tiled=True, axis_index_groups=planes
        )

    def hand_round(value):
        return [
            lax.ppermute(
                value,
                "fs",
                [
                    (e * copies + c, e * copies + (c + step) % copies)
                    for e in range(experts)
                    for c in range(copies)
                ],
            )
            for step in range(1, copies)
        ]

    def other_core(value):
        return lax.ppermute(value, "tp", [(0, 1), (1, 0)])

    def join_cols(part):
        if tp_count == 2:
            other = other_core(part)
            return jnp.where(
                tp_index == 0,
                jnp.concatenate([part, other], axis=1),
                jnp.concatenate([other, part], axis=1),
            )
        return lax.all_gather(part, "tp", axis=1, tiled=True)

    cuts = [2 * depth * k // 16 // 16 * 16 for k in (0, 4, 11, 16)]
    spans = list(zip(cuts[:-1], cuts[1:]))
    sources = [gate_weight, up_weight]

    def segments(start, stop):
        found = []
        for n in range(2):
            lo, hi = max(start, n * depth), min(stop, (n + 1) * depth)
            if lo < hi:
                found.append((n, lo - n * depth, hi - lo))
        return found

    def fold(span, *earlier):
        gain = after(norm_gain, *earlier) if earlier else norm_gain
        parts = [
            (gain[None, a : a + size, None] * sources[n][:, a : a + size]).astype(jnp.bfloat16)
            for n, a, size in segments(*span)
        ]
        return jnp.concatenate(parts, axis=1) if len(parts) > 1 else parts[0]

    first_block = fold(spans[0])
    tokens, route_ids = lax.optimization_barrier((tokens, route_ids, first_block))[:2]
    names = jnp.arange(experts, dtype=jnp.int32)
    named = jnp.any(route_ids[:, :, None] == names[None, None, :], axis=1)
    row_no = jnp.arange(rows, dtype=jnp.int32)
    earlier = (row_no[:, None] > row_no[None, :]).astype(jnp.bfloat16)
    before = jnp.dot(earlier, named.astype(jnp.bfloat16), preferred_element_type=jnp.float32)
    rank = jnp.where(named, before.astype(jnp.int32), CAP)
    values = tokens.astype(jnp.float32)
    center = jnp.mean(values, axis=1, keepdims=True)
    spread = jnp.mean(jnp.square(values - center), axis=1, keepdims=True)
    normed = ((values - center) * lax.rsqrt(spread + 1e-06)).astype(jnp.bfloat16)
    own_cols = lax.dynamic_slice_in_dim(normed, tp_index * share_width, share_width, 1)
    extra = jnp.pad(rank.astype(jnp.bfloat16), ((0, 0), (0, 128 - experts)))
    chunk = jnp.concatenate([own_cols, extra], axis=1)

    inner = 2 if copies == 2 else 1
    line = experts // inner
    spot_z = expert // inner
    spot_y = expert % inner

    def along_line(value, step):
        return lax.ppermute(
            value,
            "fs",
            [
                ((z * inner + y) * copies + c, ((z + step) * inner + y) * copies + c)
                for z in range(line)
                if 0 <= z + step < line
                for y in range(inner)
                for c in range(copies)
            ],
        )

    def across(value):
        return lax.ppermute(
            value,
            "fs",
            [
                ((z * inner + y) * copies + c, (z * inner + 1 - y) * copies + c)
                for z in range(line)
                for y in range(inner)
                for c in range(copies)
            ],
        )

    rising = [chunk]
    falling = [chunk]
    for _ in range(1, line):
        rising.append(along_line(rising[-1], 1))
        falling.append(along_line(falling[-1], -1))

    def near(k):
        return jnp.where(spot_z >= k, rising[k], falling[line - k])

    middle = line // 2
    ends = [k for k in range(1, line) if k != middle]
    near_middle = near(middle)
    near_ends = jnp.stack([near(k) for k in ends])
    arrays = [chunk[None], near_middle[None], near_ends]
    if inner == 2:
        far_own = across(chunk)
        far_middle = across(near_middle)
        far_ends = across(near_ends)
        arrays += [far_own[None], far_middle[None], far_ends]
    layout = []
    order = []
    for g in range(inner):
        for k in range(line):
            at = 0 if k == 0 else 1 if k == middle else 2
            layout.append((3 * g + at, ends.index(k) if at == 2 else 0))
            order.append((spot_z - k) % line * inner + (spot_y if g == 0 else 1 - spot_y))
    where = jnp.stack(order + [expert]).astype(jnp.int32)
    piece_cols = pick_rows(arrays, layout, where, share_width)
    piece_cols = piece_cols.reshape(experts * CAP, share_width)
    piece = join_cols(piece_cols)

    spots = jnp.stack(
        [e * copies + (lane - c) % copies for c in range(copies) for e in range(experts)]
    ).astype(jnp.int32)
    shape = (fs_count, depth, cols)
    held = []
    for n, span in enumerate(spans):
        block = first_block if n == 0 else fold(span, chunk)
        if n:
            block = after(block, held[-1][0])
        own = exchange(block)
        held.append([own] + hand_round(own))
    made = []
    for target in range(2):
        parts = []
        moves = []
        for n, span in enumerate(spans):
            first = 0
            for tensor, start, size in segments(*span):
                if tensor == target:
                    moves += [
                        (len(parts) + c, e, first, size, 0, start, c * experts + e)
                        for c in range(copies)
                        for e in range(experts)
                    ]
                    parts += held[n]
                first += size
        made += place(parts, moves, spots, [shape])
    gate_new, up_new = (m.reshape(1, width, cols) for m in made)

    gate_act = jnp.dot(piece, gate_new[0], preferred_element_type=jnp.float32)
    up_act = jnp.dot(piece, up_new[0], preferred_element_type=jnp.float32)
    hidden = (jax.nn.silu(gate_act) * up_act).astype(jnp.bfloat16)
    hidden = after(hidden)

    cuts = [depth * k // 8 for k in (0, 4, 8)]
    spans = list(zip(cuts[:-1], cuts[1:]))
    groups = []
    for n, (start, stop) in enumerate(spans):
        send = after(down_weight[:, start:stop].astype(jnp.bfloat16), chunk)
        send = after(send, groups[-1][0] if n else held[-1][0])
        own = exchange(send)
        groups.append([own] + hand_round(own))
    moves = [
        (g * copies + c, e, 0, stop - start, 0, start, c * experts + e)
        for g, (start, stop) in enumerate(spans)
        for c in range(copies)
        for e in range(experts)
    ]
    (down_new,) = place([a for group in groups for a in group], moves, spots, [shape])
    down_new = down_new.reshape(1, width, cols)

    tenth = experts // tp_count

    def project(group):
        def part(index):
            matrix = jnp.concatenate(
                [lax.dynamic_slice_in_dim(a, index * tenth, tenth, 0) for a in group], axis=0
            ).reshape(-1, cols)
            return jnp.einsum(
                "rf,df->rd", hidden, matrix, preferred_element_type=jnp.float32
            ).astype(jnp.bfloat16)

        if tp_count == 2:
            given = part(1 - tp_index)
            came = other_core(given)
            kept = after(part(tp_index), given)
            share = (kept.astype(jnp.float32) + came.astype(jnp.float32)).astype(
                jnp.bfloat16
            )
        else:
            partial = jnp.concatenate([part(t) for t in range(tp_count)], axis=1)
            share = lax.psum_scatter(partial, "tp", scatter_dimension=1, tiled=True)
        return share.reshape(experts, CAP, -1)

    backs = []
    shares = [hidden]
    for n, group in enumerate(groups):
        group = [after(a, shares[-1]) for a in group]
        shares.append(project(group))
        share = after(shares[-1], backs[-1] if n else groups[-1][0])
        backs.append(exchange(share))

    def hot_rows(k):
        spot = jnp.sum(
            jnp.where(route_ids[:, k, None] == names[None, :], rank + CAP * names[None, :], 0),
            axis=1,
        )
        return (spot[:, None] == jnp.arange(experts * CAP, dtype=jnp.int32)[None, :]).astype(
            jnp.bfloat16
        )

    hot = [hot_rows(0), hot_rows(1)]
    first_weight = jax.nn.sigmoid(route_logits[:, 0] - route_logits[:, 1])[:, None]
    second_weight = jax.nn.sigmoid(route_logits[:, 1] - route_logits[:, 0])[:, None]

    def mix(back):
        back = back.reshape(experts * CAP, -1)
        first, second = (jnp.dot(h, back, preferred_element_type=jnp.float32) for h in hot)
        return (first_weight * first + second_weight * second).astype(jnp.bfloat16)

    order = jnp.concatenate(
        [
            (
                (
                    (jnp.arange(tenth)[None, :, None] * copies)
                    + (lane - jnp.arange(copies)[:, None, None]) % copies
                )
                * depth
                + start
                + jnp.arange(stop - start)[None, None, :]
            ).reshape(-1)
            for start, stop in spans
        ]
    )
    in_order = (order[:, None] == jnp.arange(share_width)[None, :]).astype(jnp.bfloat16)
    mixed_cols = jnp.concatenate([mix(back) for back in backs], axis=1)
    mixed_cols = jnp.dot(mixed_cols, in_order, preferred_element_type=jnp.float32)
    mixed = join_cols(mixed_cols.astype(jnp.bfloat16))
    return (mixed, gate_new, up_new, down_new)


def solution(mesh):
    return jax.shard_map(
        body,
        mesh=mesh,
        in_specs=(
            P("fs", None),
            P("fs", None),
            P("fs", None),
            P("fs"),
            P(None, "fs", "tp"),
            P(None, "fs", "tp"),
            P(None, "fs", "tp"),
        ),
        out_specs=(P("fs", None), P("fs", None, "tp"), P("fs", None, "tp"), P("fs", None, "tp")),
        check_vma=False,
    )
```

```python
import functools

import jax
import jax.numpy as jnp
import numpy as np
from jax import lax
from jax.experimental import pallas as pl
from jax.experimental.pallas import tpu as pltpu
from jax.sharding import PartitionSpec as P

CAP = 96


def after(value, *earlier):
    return lax.optimization_barrier((value,) + earlier)[0]


def place_kernel(moves, number, where_ref, *refs):
    arrays, outs = refs[:number], refs[number : -2 - number]
    held = refs[-2 - number : -2]
    in_sems, out_sems = refs[-2:]
    loads = [
        pltpu.make_async_copy(array, held[i], in_sems.at[i]) for i, array in enumerate(arrays)
    ]
    for load in loads:
        load.start()
    stores = []
    seen = set()
    for n, (i, part, first, rows, out, start, slot) in enumerate(moves):
        if i not in seen:
            loads[i].wait()
            seen.add(i)
        store = pltpu.make_async_copy(
            held[i].at[part, pl.ds(first, rows)],
            outs[out].at[where_ref[slot], pl.ds(start, rows)],
            out_sems.at[n],
        )
        store.start()
        stores.append(store)
    for store in stores:
        store.wait()


def place(arrays, moves, where, out_shapes):
    dtype = arrays[0].dtype
    hbm = pl.BlockSpec(memory_space=pltpu.HBM)
    size = 2 * sum(int(np.prod(a.shape)) for a in arrays)
    return pl.pallas_call(
        functools.partial(place_kernel, moves, len(arrays)),
        grid_spec=pltpu.PrefetchScalarGridSpec(
            num_scalar_prefetch=1,
            grid=(),
            in_specs=[hbm] * len(arrays),
            out_specs=[hbm] * len(out_shapes),
            scratch_shapes=[pltpu.VMEM(a.shape, dtype) for a in arrays]
            + [
                pltpu.SemaphoreType.DMA((len(arrays),)),
                pltpu.SemaphoreType.DMA((len(moves),)),
            ],
        ),
        out_shape=[jax.ShapeDtypeStruct(s, dtype) for s in out_shapes],
        cost_estimate=pl.CostEstimate(flops=4 * size, bytes_accessed=2 * size, transcendentals=0),
    )(where, *arrays)


def pick_kernel(layout, cols, where_ref, *refs):
    arrays, out_ref = refs[:-1], refs[-1]
    expert = where_ref[len(layout)]
    slots = lax.broadcasted_iota(jnp.int32, (1, CAP), 1).astype(jnp.float32)
    for n, (i, part) in enumerate(layout):
        block = arrays[i][part]
        extra = block[:, cols:].astype(jnp.float32)
        column = lax.broadcasted_iota(jnp.int32, extra.shape, 1)
        rank = jnp.sum(jnp.where(column == expert, extra, 0.0), axis=1, keepdims=True)
        hot = (rank == slots).astype(jnp.float32).astype(block.dtype)
        rows = lax.dot_general(
            hot, block[:, :cols], (((0,), (0,)), ((), ())), preferred_element_type=jnp.float32
        )
        out_ref[where_ref[n]] = rows.astype(out_ref.dtype)


def pick_rows(arrays, layout, where, cols):
    size = 2 * sum(int(np.prod(a.shape)) for a in arrays)
    rows = arrays[0].shape[1]
    vmem = pl.BlockSpec(memory_space=pltpu.VMEM)
    return pl.pallas_call(
        functools.partial(pick_kernel, layout, cols),
        grid_spec=pltpu.PrefetchScalarGridSpec(
            num_scalar_prefetch=1, grid=(), in_specs=[vmem] * len(arrays), out_specs=vmem
        ),
        out_shape=jax.ShapeDtypeStruct((len(layout), CAP, cols), arrays[0].dtype),
        cost_estimate=pl.CostEstimate(
            flops=2 * len(layout) * CAP * rows * cols, bytes_accessed=2 * size, transcendentals=0
        ),
    )(where, *arrays)


def body(tokens, route_ids, route_logits, norm_gain, gate_weight, up_weight, down_weight):
    experts, depth, cols = gate_weight.shape
    fs_count = lax.axis_size("fs")
    tp_count = lax.axis_size("tp")
    copies = fs_count // experts
    rows, width = tokens.shape
    share_width = width // tp_count
    lane = lax.axis_index("fs") % copies
    expert = lax.axis_index("fs") // copies
    tp_index = lax.axis_index("tp")
    planes = [[e * copies + c for e in range(experts)] for c in range(copies)]

    def exchange(value):
        return lax.all_to_all(
            value, "fs", split_axis=0, concat_axis=0, tiled=True, axis_index_groups=planes
        )

    def hand_round(value):
        return [
            lax.ppermute(
                value,
                "fs",
                [
                    (e * copies + c, e * copies + (c + step) % copies)
                    for e in range(experts)
                    for c in range(copies)
                ],
            )
            for step in range(1, copies)
        ]

    def other_core(value):
        return lax.ppermute(value, "tp", [(0, 1), (1, 0)])

    def join_cols(part):
        if tp_count == 2:
            other = other_core(part)
            return jnp.where(
                tp_index == 0,
                jnp.concatenate([part, other], axis=1),
                jnp.concatenate([other, part], axis=1),
            )
        return lax.all_gather(part, "tp", axis=1, tiled=True)

    cuts = [2 * depth * k // 16 // 16 * 16 for k in (0, 5, 11, 16)]
    spans = list(zip(cuts[:-1], cuts[1:]))
    sources = [gate_weight, up_weight]

    def segments(start, stop):
        found = []
        for n in range(2):
            lo, hi = max(start, n * depth), min(stop, (n + 1) * depth)
            if lo < hi:
                found.append((n, lo - n * depth, hi - lo))
        return found

    def fold(span, *earlier):
        gain = after(norm_gain, *earlier) if earlier else norm_gain
        parts = [
            (gain[None, a : a + size, None] * sources[n][:, a : a + size]).astype(jnp.bfloat16)
            for n, a, size in segments(*span)
        ]
        return jnp.concatenate(parts, axis=1) if len(parts) > 1 else parts[0]

    first_block = fold(spans[0])
    tokens, route_ids = lax.optimization_barrier((tokens, route_ids, first_block))[:2]
    tokens, route_ids = lax.optimization_barrier((tokens, route_ids, first_block))[:2]
    block_expert = np.tile(np.arange(experts, dtype=np.int32), copies)
    block_copy = np.repeat(np.arange(copies, dtype=np.int32), experts)

    def moves_of(groups, pieces):
        arrays, moves = [], []
        for n, first, size, start in pieces:
            moves += [
                (len(arrays) + c, e, first, size, 0, start, c * experts + e)
                for c in range(copies)
                for e in range(experts)
            ]
            arrays += groups[n]
        return arrays, moves

    names = jnp.arange(experts, dtype=jnp.int32)
    named = jnp.any(route_ids[:, :, None] == names[None, None, :], axis=1)
    row_no = jnp.arange(rows, dtype=jnp.int32)
    earlier = (row_no[:, None] > row_no[None, :]).astype(jnp.bfloat16)
    before = jnp.dot(earlier, named.astype(jnp.bfloat16), preferred_element_type=jnp.float32)
    rank = jnp.where(named, before.astype(jnp.int32), CAP)
    values = tokens.astype(jnp.float32)
    center = jnp.mean(values, axis=1, keepdims=True)
    spread = jnp.mean(jnp.square(values - center), axis=1, keepdims=True)
    normed = ((values - center) * lax.rsqrt(spread + 1e-06)).astype(jnp.bfloat16)
    own_cols = lax.dynamic_slice_in_dim(normed, tp_index * share_width, share_width, 1)
    extra = jnp.pad(rank.astype(jnp.bfloat16), ((0, 0), (0, 128 - experts)))
    chunk = jnp.concatenate([own_cols, extra], axis=1)

    inner = 2 if copies == 2 else 1
    line = experts // inner
    spot_z = expert // inner
    spot_y = expert % inner

    def along_line(value, step):
        return lax.ppermute(
            value,
            "fs",
            [
                ((z * inner + y) * copies + c, ((z + step) * inner + y) * copies + c)
                for z in range(line)
                if 0 <= z + step < line
                for y in range(inner)
                for c in range(copies)
            ],
        )

    def across(value):
        return lax.ppermute(
            value,
            "fs",
            [
                ((z * inner + y) * copies + c, (z * inner + 1 - y) * copies + c)
                for z in range(line)
                for y in range(inner)
                for c in range(copies)
            ],
        )

    rising = [chunk]
    falling = [chunk]
    for _ in range(1, line):
        rising.append(along_line(rising[-1], 1))
        falling.append(along_line(falling[-1], -1))
    sides = [chunk]
    if line == 4:
        table = np.array([[0, 1, 2, 3], [1, 0, 3, 2], [2, 1, 0, 3], [3, 2, 1, 0]], np.int32)
        first, last = spot_z == 0, spot_z == line - 1
        sides.append(jnp.where(first, falling[1], rising[1]))
        low = spot_z < 2
        high_value = after(rising[2], sides[1])
        sides.append(jnp.where(low, falling[2], high_value))
        top = after(rising[3], sides[1], sides[2])
        outer = jnp.where(first, falling[3], jnp.where(last, top, falling[1]))
        sides.append(outer)
    else:
        table = np.array([[(z - k) % line for k in range(line)] for z in range(line)], np.int32)
        for k in range(1, line):
            sides.append(jnp.where(spot_z >= k, rising[k], falling[line - k]))
    arrays = [value[None] for value in sides]
    lines = jnp.sum(jnp.where(jnp.arange(line)[:, None] == spot_z, table, 0), axis=0)
    order = [lines * inner + spot_y]
    if inner == 2:
        for value in sides:
            arrays.append(across(value)[None])
        order.append(lines * inner + 1 - spot_y)
    layout = [(n, 0) for n in range(len(arrays))]
    where = jnp.concatenate(order + [expert[None]]).astype(jnp.int32)
    piece_cols = pick_rows(arrays, layout, where, share_width)
    piece_cols = piece_cols.reshape(experts * CAP, share_width)
    piece = join_cols(piece_cols)

    spots = (block_expert * copies + (lane - block_copy) % copies).astype(jnp.int32)
    shape = (fs_count, depth, cols)
    held = []
    for n, span in enumerate(spans):
        block = first_block if n == 0 else fold(span, chunk)
        if n:
            block = after(block, held[-1][0])
        own = exchange(block)
        held.append([own] + hand_round(own))
    made = []
    for target in range(2):
        pieces = []
        for n, span in enumerate(spans):
            first = 0
            for tensor, start, size in segments(*span):
                if tensor == target:
                    pieces.append((n, first, size, start))
                first += size
        parts, moves = moves_of(held, pieces)
        made += place(parts, moves, spots, [shape])
    gate_new, up_new = (m.reshape(1, width, cols) for m in made)

    gate_act = jnp.dot(piece, gate_new[0], preferred_element_type=jnp.float32)
    up_act = jnp.dot(piece, up_new[0], preferred_element_type=jnp.float32)
    hidden = (jax.nn.silu(gate_act) * up_act).astype(jnp.bfloat16)
    hidden = after(hidden)

    cuts = [depth * k // 8 for k in (0, 4, 8)]
    spans = list(zip(cuts[:-1], cuts[1:]))
    groups = []
    for n, (start, stop) in enumerate(spans):
        send = after(down_weight[:, start:stop].astype(jnp.bfloat16), chunk)
        send = after(send, groups[-1][0] if n else held[-1][0])
        own = exchange(send)
        groups.append([own] + hand_round(own))
    parts, moves = moves_of(
        groups, [(g, 0, stop - start, start) for g, (start, stop) in enumerate(spans)]
    )
    (down_new,) = place(parts, moves, spots, [shape])
    down_new = down_new.reshape(1, width, cols)

    tenth = experts // tp_count

    def times(matrix):
        return jnp.einsum(
            "rf,df->rd", hidden, matrix.reshape(-1, cols), preferred_element_type=jnp.float32
        ).astype(jnp.bfloat16)

    def shared(part, *earlier):
        if tp_count == 2:
            given = times(part(1 - tp_index, *earlier))
            came = other_core(given)
            kept = after(times(part(tp_index, given)), given)
            share = (kept.astype(jnp.float32) + came.astype(jnp.float32)).astype(jnp.bfloat16)
        else:
            partial = jnp.concatenate([times(part(t)) for t in range(tp_count)], axis=1)
            share = lax.psum_scatter(partial, "tp", scatter_dimension=1, tiled=True)
        return share.reshape(experts, CAP, -1)

    def blocks(copy_range, index, *earlier):
        return jnp.concatenate(
            [
                lax.dynamic_slice_in_dim(
                    after(group[c], *earlier) if earlier else group[c], index * tenth, tenth, 0
                ).reshape(-1, cols)
                for group in groups
                for c in copy_range
            ]
        )

    def own_part(index, *earlier):
        return blocks(range(1), index)

    def rest_part(index, *earlier):
        return blocks(range(1, copies), index, *earlier)

    share_own = shared(own_part)
    share_own = after(share_own, groups[-1][0])
    back_own = exchange(share_own)
    share_rest = after(shared(rest_part, share_own), back_own)
    back_rest = exchange(share_rest)
    backs = [back_own, back_rest]

    def hot_rows(k):
        spot = jnp.sum(
            jnp.where(route_ids[:, k, None] == names[None, :], rank + CAP * names[None, :], 0),
            axis=1,
        )
        return (spot[:, None] == jnp.arange(experts * CAP, dtype=jnp.int32)[None, :]).astype(
            jnp.bfloat16
        )

    hot = [hot_rows(0), hot_rows(1)]
    first_weight = jax.nn.sigmoid(route_logits[:, 0] - route_logits[:, 1])[:, None]
    second_weight = jax.nn.sigmoid(route_logits[:, 1] - route_logits[:, 0])[:, None]

    def mix(back):
        back = back.reshape(experts * CAP, -1)
        first, second = (jnp.dot(h, back, preferred_element_type=jnp.float32) for h in hot)
        return (first_weight * first + second_weight * second).astype(jnp.bfloat16)

    order = jnp.concatenate(
        [
            (
                (
                    (jnp.arange(tenth)[None, :, None] * copies)
                    + (lane - jnp.arange(lo, hi)[:, None, None]) % copies
                )
                * depth
                + start
                + jnp.arange(stop - start)[None, None, :]
            ).reshape(-1)
            for lo, hi in ((0, 1), (1, copies))
            for start, stop in spans
        ]
    )
    in_order = (order[:, None] == jnp.arange(share_width)[None, :]).astype(jnp.bfloat16)
    mixed_cols = jnp.concatenate([mix(back) for back in backs], axis=1)
    mixed_cols = jnp.dot(mixed_cols, in_order, preferred_element_type=jnp.float32)
    mixed = join_cols(mixed_cols.astype(jnp.bfloat16))
    return (mixed, gate_new, up_new, down_new)


def solution(mesh):
    return jax.shard_map(
        body,
        mesh=mesh,
        in_specs=(
            P("fs", None),
            P("fs", None),
            P("fs", None),
            P("fs"),
            P(None, "fs", "tp"),
            P(None, "fs", "tp"),
            P(None, "fs", "tp"),
        ),
        out_specs=(P("fs", None), P("fs", None, "tp"), P("fs", None, "tp"), P("fs", None, "tp")),
        check_vma=False,
    )
```

```python
import functools

import jax
import jax.numpy as jnp
import numpy as np
from jax import lax
from jax.experimental import pallas as pl
from jax.experimental.pallas import tpu as pltpu
from jax.sharding import PartitionSpec as P

CAP = 96


def after(value, *earlier):
    return lax.optimization_barrier((value,) + earlier)[0]


def place_kernel(moves, number, where_ref, *refs):
    arrays, outs = refs[:number], refs[number : -2 - number]
    held = refs[-2 - number : -2]
    in_sems, out_sems = refs[-2:]
    loads = [
        pltpu.make_async_copy(array, held[i], in_sems.at[i]) for i, array in enumerate(arrays)
    ]
    for load in loads:
        load.start()
    stores = []
    seen = set()
    for n, (i, part, first, rows, out, start, slot) in enumerate(moves):
        if i not in seen:
            loads[i].wait()
            seen.add(i)
        store = pltpu.make_async_copy(
            held[i].at[part, pl.ds(first, rows)],
            outs[out].at[where_ref[slot], pl.ds(start, rows)],
            out_sems.at[n],
        )
        store.start()
        stores.append(store)
    for store in stores:
        store.wait()


def place(arrays, moves, where, out_shapes):
    dtype = arrays[0].dtype
    hbm = pl.BlockSpec(memory_space=pltpu.HBM)
    size = 2 * sum(int(np.prod(a.shape)) for a in arrays)
    return pl.pallas_call(
        functools.partial(place_kernel, moves, len(arrays)),
        grid_spec=pltpu.PrefetchScalarGridSpec(
            num_scalar_prefetch=1,
            grid=(),
            in_specs=[hbm] * len(arrays),
            out_specs=[hbm] * len(out_shapes),
            scratch_shapes=[pltpu.VMEM(a.shape, dtype) for a in arrays]
            + [
                pltpu.SemaphoreType.DMA((len(arrays),)),
                pltpu.SemaphoreType.DMA((len(moves),)),
            ],
        ),
        out_shape=[jax.ShapeDtypeStruct(s, dtype) for s in out_shapes],
        cost_estimate=pl.CostEstimate(flops=4 * size, bytes_accessed=2 * size, transcendentals=0),
    )(where, *arrays)


def pick_kernel(layout, cols, where_ref, *refs):
    arrays, out_ref = refs[:-1], refs[-1]
    expert = where_ref[len(layout)]
    slots = lax.broadcasted_iota(jnp.int32, (1, CAP), 1).astype(jnp.float32)
    for n, (i, part) in enumerate(layout):
        block = arrays[i][part]
        extra = block[:, cols:].astype(jnp.float32)
        column = lax.broadcasted_iota(jnp.int32, extra.shape, 1)
        rank = jnp.sum(jnp.where(column == expert, extra, 0.0), axis=1, keepdims=True)
        hot = (rank == slots).astype(jnp.float32).astype(block.dtype)
        rows = lax.dot_general(
            hot, block[:, :cols], (((0,), (0,)), ((), ())), preferred_element_type=jnp.float32
        )
        out_ref[where_ref[n]] = rows.astype(out_ref.dtype)


def pick_rows(arrays, layout, where, cols):
    size = 2 * sum(int(np.prod(a.shape)) for a in arrays)
    rows = arrays[0].shape[1]
    vmem = pl.BlockSpec(memory_space=pltpu.VMEM)
    return pl.pallas_call(
        functools.partial(pick_kernel, layout, cols),
        grid_spec=pltpu.PrefetchScalarGridSpec(
            num_scalar_prefetch=1, grid=(), in_specs=[vmem] * len(arrays), out_specs=vmem
        ),
        out_shape=jax.ShapeDtypeStruct((len(layout), CAP, cols), arrays[0].dtype),
        cost_estimate=pl.CostEstimate(
            flops=2 * len(layout) * CAP * rows * cols, bytes_accessed=2 * size, transcendentals=0
        ),
    )(where, *arrays)


def body(tokens, route_ids, route_logits, norm_gain, gate_weight, up_weight, down_weight):
    experts, depth, cols = gate_weight.shape
    fs_count = lax.axis_size("fs")
    tp_count = lax.axis_size("tp")
    copies = fs_count // experts
    rows, width = tokens.shape
    share_width = width // tp_count
    lane = lax.axis_index("fs") % copies
    expert = lax.axis_index("fs") // copies
    tp_index = lax.axis_index("tp")
    planes = [[e * copies + c for e in range(experts)] for c in range(copies)]

    def exchange(value):
        return lax.all_to_all(
            value, "fs", split_axis=0, concat_axis=0, tiled=True, axis_index_groups=planes
        )

    def hand_round(value):
        return [
            lax.ppermute(
                value,
                "fs",
                [
                    (e * copies + c, e * copies + (c + step) % copies)
                    for e in range(experts)
                    for c in range(copies)
                ],
            )
            for step in range(1, copies)
        ]

    def other_core(value):
        return lax.ppermute(value, "tp", [(0, 1), (1, 0)])

    def join_cols(part):
        if tp_count == 2:
            other = other_core(part)
            whole = jnp.concatenate([part, part], axis=1)
            return lax.dynamic_update_slice_in_dim(
                whole, other, (1 - tp_index) * part.shape[1], axis=1
            )
        return lax.all_gather(part, "tp", axis=1, tiled=True)

    cuts = [2 * depth * k // 16 // 16 * 16 for k in (0, 7, 12, 16)]
    spans = list(zip(cuts[:-1], cuts[1:]))
    sources = [gate_weight, up_weight]

    def segments(start, stop):
        found = []
        for n in range(2):
            lo, hi = max(start, n * depth), min(stop, (n + 1) * depth)
            if lo < hi:
                found.append((n, lo - n * depth, hi - lo))
        return found

    def fold(span, *earlier):
        gain = after(norm_gain, *earlier) if earlier else norm_gain
        parts = [
            (gain[None, a : a + size, None] * sources[n][:, a : a + size]).astype(jnp.bfloat16)
            for n, a, size in segments(*span)
        ]
        return jnp.concatenate(parts, axis=1) if len(parts) > 1 else parts[0]

    first_block = fold(spans[0])
    tokens, route_ids = lax.optimization_barrier((tokens, route_ids, first_block))[:2]
    tokens, route_ids = lax.optimization_barrier((tokens, route_ids, first_block))[:2]
    block_expert = np.tile(np.arange(experts, dtype=np.int32), copies)
    block_copy = np.repeat(np.arange(copies, dtype=np.int32), experts)

    def moves_of(groups, pieces):
        arrays, moves = [], []
        for n, first, size, start in pieces:
            moves += [
                (len(arrays) + c, e, first, size, 0, start, c * experts + e)
                for c in range(copies)
                for e in range(experts)
            ]
            arrays += groups[n]
        return arrays, moves

    names = jnp.arange(experts, dtype=jnp.int32)
    named = jnp.any(route_ids[:, :, None] == names[None, None, :], axis=1)
    row_no = jnp.arange(rows, dtype=jnp.int32)
    earlier = (row_no[:, None] > row_no[None, :]).astype(jnp.bfloat16)
    before = jnp.dot(earlier, named.astype(jnp.bfloat16), preferred_element_type=jnp.float32)
    rank = jnp.where(named, before.astype(jnp.int32), CAP)
    values = tokens.astype(jnp.float32)
    center = jnp.mean(values, axis=1, keepdims=True)
    spread = jnp.mean(jnp.square(values - center), axis=1, keepdims=True)
    normed = ((values - center) * lax.rsqrt(spread + 1e-06)).astype(jnp.bfloat16)
    own_cols = lax.dynamic_slice_in_dim(normed, tp_index * share_width, share_width, 1)
    extra = jnp.pad(rank.astype(jnp.bfloat16), ((0, 0), (0, 128 - experts)))
    chunk = jnp.concatenate([own_cols, extra], axis=1)

    inner = 2 if copies == 2 else 1
    line = experts // inner
    spot_z = expert // inner
    spot_y = expert % inner

    def along_line(value, step):
        return lax.ppermute(
            value,
            "fs",
            [
                ((z * inner + y) * copies + c, ((z + step) * inner + y) * copies + c)
                for z in range(line)
                if 0 <= z + step < line
                for y in range(inner)
                for c in range(copies)
            ],
        )

    def across(value):
        return lax.ppermute(
            value,
            "fs",
            [
                ((z * inner + y) * copies + c, (z * inner + 1 - y) * copies + c)
                for z in range(line)
                for y in range(inner)
                for c in range(copies)
            ],
        )

    rising = [chunk]
    falling = [chunk]
    for _ in range(1, line):
        rising.append(along_line(rising[-1], 1))
        falling.append(along_line(falling[-1], -1))
    sides = [chunk]
    if line == 4:
        table = np.array([[0, 1, 2, 3], [1, 0, 3, 2], [2, 1, 0, 3], [3, 2, 1, 0]], np.int32)
        first, last = spot_z == 0, spot_z == line - 1
        sides.append(jnp.where(first, falling[1], rising[1]))
        low = spot_z < 2
        high_value = after(rising[2], sides[1])
        sides.append(jnp.where(low, falling[2], high_value))
        top = after(rising[3], sides[1], sides[2])
        outer = jnp.where(first, falling[3], jnp.where(last, top, falling[1]))
        sides.append(outer)
    else:
        table = np.array([[(z - k) % line for k in range(line)] for z in range(line)], np.int32)
        for k in range(1, line):
            sides.append(jnp.where(spot_z >= k, rising[k], falling[line - k]))
    arrays = [value[None] for value in sides]
    lines = jnp.sum(jnp.where(jnp.arange(line)[:, None] == spot_z, table, 0), axis=0)
    order = [lines * inner + spot_y]
    if inner == 2:
        for value in sides:
            arrays.append(across(value)[None])
        order.append(lines * inner + 1 - spot_y)
    layout = [(n, 0) for n in range(len(arrays))]
    where = jnp.concatenate(order + [expert[None]]).astype(jnp.int32)
    piece_cols = pick_rows(arrays, layout, where, share_width)
    piece_cols = piece_cols.reshape(experts * CAP, share_width)
    piece = after(join_cols(piece_cols))

    spots = (block_expert * copies + (lane - block_copy) % copies).astype(jnp.int32)
    shape = (fs_count, depth, cols)
    held = []
    for n, span in enumerate(spans):
        block = first_block if n == 0 else fold(span, chunk)
        if n:
            block = after(block, held[-1][0])
        own = exchange(block)
        held.append([own] + hand_round(own))
    made = []
    for target in range(2):
        pieces = []
        for n, span in enumerate(spans):
            first = 0
            for tensor, start, size in segments(*span):
                if tensor == target:
                    pieces.append((n, first, size, start))
                first += size
        parts, moves = moves_of(held, pieces)
        made += place(parts, moves, spots, [shape])
    gate_new, up_new = (m.reshape(1, width, cols) for m in made)

    gate_act = jnp.dot(piece, gate_new[0], preferred_element_type=jnp.float32)
    up_act = jnp.dot(piece, up_new[0], preferred_element_type=jnp.float32)
    hidden = (jax.nn.silu(gate_act) * up_act).astype(jnp.bfloat16)
    hidden = after(hidden)

    cuts = [depth * k // 8 for k in (0, 4, 8)]
    spans = list(zip(cuts[:-1], cuts[1:]))
    groups = []
    for n, (start, stop) in enumerate(spans):
        send = after(down_weight[:, start:stop].astype(jnp.bfloat16), chunk)
        send = after(send, groups[-1][0] if n else held[-1][0])
        own = exchange(send)
        groups.append([own] + hand_round(own))
    parts, moves = moves_of(
        groups, [(g, 0, stop - start, start) for g, (start, stop) in enumerate(spans)]
    )
    (down_new,) = place(parts, moves, spots, [shape])
    down_new = down_new.reshape(1, width, cols)

    tenth = experts // tp_count

    def times(matrix):
        return jnp.einsum(
            "rf,df->rd", hidden, matrix.reshape(-1, cols), preferred_element_type=jnp.float32
        ).astype(jnp.bfloat16)

    def shared(part, *earlier):
        if tp_count == 2:
            given = times(part(1 - tp_index, *earlier))
            came = other_core(given)
            kept = after(times(part(tp_index, given)), given)
            share = (kept.astype(jnp.float32) + came.astype(jnp.float32)).astype(jnp.bfloat16)
        else:
            partial = jnp.concatenate([times(part(t)) for t in range(tp_count)], axis=1)
            share = lax.psum_scatter(partial, "tp", scatter_dimension=1, tiled=True)
        return share.reshape(experts, CAP, -1)

    def blocks(copy_range, index, *earlier):
        return jnp.concatenate(
            [
                lax.dynamic_slice_in_dim(
                    after(group[c], *earlier) if earlier else group[c], index * tenth, tenth, 0
                ).reshape(-1, cols)
                for group in groups
                for c in copy_range
            ]
        )

    def own_part(index, *earlier):
        return blocks(range(1), index)

    def rest_part(index, *earlier):
        return blocks(range(1, copies), index, *earlier)

    share_own = shared(own_part)
    share_own = after(share_own, groups[-1][0])
    back_own = exchange(share_own)
    share_rest = after(shared(rest_part, share_own), back_own)
    back_rest = exchange(share_rest)
    backs = [back_own, back_rest]

    def hot_rows(k):
        spot = jnp.sum(
            jnp.where(route_ids[:, k, None] == names[None, :], rank + CAP * names[None, :], 0),
            axis=1,
        )
        return (spot[:, None] == jnp.arange(experts * CAP, dtype=jnp.int32)[None, :]).astype(
            jnp.bfloat16
        )

    hot = [hot_rows(0), hot_rows(1)]
    first_weight = jax.nn.sigmoid(route_logits[:, 0] - route_logits[:, 1])[:, None]
    second_weight = jax.nn.sigmoid(route_logits[:, 1] - route_logits[:, 0])[:, None]

    def mix(back):
        back = back.reshape(experts * CAP, -1)
        first, second = (jnp.dot(h, back, preferred_element_type=jnp.float32) for h in hot)
        return (first_weight * first + second_weight * second).astype(jnp.bfloat16)

    order = jnp.concatenate(
        [
            (
                (
                    (jnp.arange(tenth)[None, :, None] * copies)
                    + (lane - jnp.arange(lo, hi)[:, None, None]) % copies
                )
                * depth
                + start
                + jnp.arange(stop - start)[None, None, :]
            ).reshape(-1)
            for lo, hi in ((0, 1), (1, copies))
            for start, stop in spans
        ]
    )
    in_order = (order[:, None] == jnp.arange(share_width)[None, :]).astype(jnp.bfloat16)
    mixed_cols = jnp.concatenate([mix(back) for back in backs], axis=1)
    mixed_cols = jnp.dot(mixed_cols, in_order, preferred_element_type=jnp.float32)
    mixed = join_cols(mixed_cols.astype(jnp.bfloat16))
    return (mixed, gate_new, up_new, down_new)


def solution(mesh):
    return jax.shard_map(
        body,
        mesh=mesh,
        in_specs=(
            P("fs", None),
            P("fs", None),
            P("fs", None),
            P("fs"),
            P(None, "fs", "tp"),
            P(None, "fs", "tp"),
            P(None, "fs", "tp"),
        ),
        out_specs=(P("fs", None), P("fs", None, "tp"), P("fs", None, "tp"), P("fs", None, "tp")),
        check_vma=False,
    )
```
